32 devices in a mesh: sp: 16 (over z, y, core), tp: 2 (over x).
Axes of the slice: x: 2, y: 2, z: 4, core: 2. Of those that a mesh axis runs over, the one named last changes fastest.
Arguments:
- pool_input: bfloat16 [4, 128, 8192], P(None, 'tp', 'sp'), may hold values from -8 to 8
- doc_ids: int32 [8192], P('sp'), may hold values from 0 to 3, never falling along the last dimension, each value on 1 to 4096 neighbouring positions
- pool_map: bfloat16 [4, 128, 128], replicated, may hold values from -0.5 to 0.5
- pool_scale: float32 [512], replicated, may hold values from 0.1 to 1.9
- w_out: bfloat16 [512, 2048], replicated, may hold values from -0.25 to 0.25
- residual: bfloat16 [8192, 2048], P(('sp', 'tp')), may hold values from -6 to 6
- mix_gain: float32 [2048], replicated, may hold values from 0.1 to 1.9
- ffn_gain: float32 [2048], replicated, may hold values from 0.1 to 1.9
- out_gain: float32 [2048], replicated, may hold values from 0.1 to 1.9
- expert_ids: int32 [8192, 2], P(('sp', 'tp')), may hold values from 0 to 31, all different within a row; in each aligned block of 256 rows (0 to 255, 256 to 511, ...) at most 32 rows name the same one
- route_logits: float32 [8192, 2], P(('sp', 'tp')), may hold values from -6 to 6
- w_gate: bfloat16 [32, 2048, 1024], P(('sp', 'tp')), may hold values from -0.125 to 0.125
- w_up: bfloat16 [32, 2048, 1024], P(('sp', 'tp')), may hold values from -0.125 to 0.125
- w_down: bfloat16 [32, 1024, 2048], P(('sp', 'tp')), may hold values from -0.1875 to 0.1875
Outputs:
- layer_out: bfloat16 [8192, 2048], P(('sp', 'tp'))
The draws below stay inside these ranges and needn't reach their ends.
Inputs may be any that keep to these rules, and one draw needn't show every extreme that they name: `doc_ids`: document numbers never fall along the positions; no document has more than 4096 positions. `expert_ids`: each row names 2 different experts; within each aligned block of 256 rows no expert is named by more than 32 rows, a bound that some block reaches.
All inputs are finite; a program needn't handle non-finite values.
Results may differ from the reference program's by a relative error of at most 0.03.
Values may be sent and summed in bfloat16 or wider, within the bound.
No kernel may reach another device: no remote copies, remote signals or barrier semaphores. Data moves between devices by JAX's collectives and lax.ppermute only.
A program may use at most 64 MiB of HBM per device.

```python
import math
import jax
import jax.numpy as jnp
import numpy as np
from jax import lax

D = 2048
FF = 1024
GROUPS = 4
GROUP_W = 128
TOP_K = 2
TOK_DEV = 512
POOL_W = 512
TOKENS = 8192
ROWS_DEV = 256
EXPERTS = 32
CAP = 32
DOCS = 4
DOC_MOST = 4096
DEVICES = 32


def draw_pool_input(key, part):
    noise_key = jax.random.fold_in(key, 11)
    level_key = jax.random.fold_in(key, 12)
    span_len = max(TOK_DEV // 2, 1)
    span_count = TOKENS // span_len
    noise = jax.random.normal(noise_key, (GROUPS, GROUP_W, TOKENS), jnp.float32)
    levels = jax.random.normal(level_key, (GROUPS, GROUP_W, span_count), jnp.float32)
    full = noise + jnp.repeat(levels, span_len, axis=2)
    return jnp.clip(full, -8.0, 8.0).astype(jnp.bfloat16)


def block_scale(key, extent, pieces, low, largest):
    def one(dim, parts):
        heights = jax.random.uniform(jax.random.fold_in(jax.random.fold_in(key, 6), dim), (parts,), jnp.float32, low / len(pieces), largest / len(pieces))
        return jnp.repeat(jnp.exp(heights), extent[dim] // parts).reshape((-1,) + (1,) * (len(extent) - dim - 1))

    loudness = one(*pieces[0])
    for cut in pieces[1:]:
        loudness = loudness * one(*cut)
    return loudness


def split_up(count, total, reach, lean):
    loads = [(1 << 20) // math.isqrt(rank ** lean) + 1 for rank in range(2, count + 1)]
    surplus, given = total - reach - (count - 1), [1] * (count - 1)
    while surplus > 0:
        candidates = [i for i in range(count - 1) if given[i] < reach]
        whole, remaining = sum([loads[i] for i in candidates]), surplus
        for i in candidates:
            addition = min(reach - given[i], max(1, remaining * loads[i] // whole), surplus)
            given[i] = given[i] + addition
            surplus = surplus - addition
    return np.array([reach] + given)


def uneven_parts(own_key, number_of, total, bound, lean):
    if number_of == 2:
        one = jax.random.randint(own_key, (), max(1, total - bound), min(bound, total - 1) + 1)
        return jnp.stack([one, total - one])
    tallies = jnp.asarray(split_up(number_of, total, bound, lean), jnp.int32)
    pairs = (number_of - 1) // 2
    giver, sink = tallies[1:1 + 2 * pairs:2], tallies[2:2 + 2 * pairs:2]
    room = jnp.minimum(giver - 1, bound - sink)
    passed = jax.random.randint(jax.random.fold_in(own_key, 1), (pairs,), 0, 1 << 20) % (room + 1)
    tallies = tallies.at[1:1 + 2 * pairs:2].set(giver - passed).at[2:2 + 2 * pairs:2].set(sink + passed)
    return tallies[jax.random.permutation(jax.random.fold_in(own_key, 2), number_of)]


def deal_out(rng, own, number, rows, amount, top, limit, slope):
    order = jax.random.permutation(rng, amount)
    crowded, ordinary = portions_of(amount, rows * top, limit, slope, True), portions_of(amount, rows * top, limit, slope, False)
    places = jnp.arange(amount)

    def named(sizes, rotation):
        used = int((sizes > 0).sum())
        fixed = max(1, used // 4)
        moved = fixed + (places - fixed + rotation * (used - fixed)) % max(1, amount - fixed)
        return jnp.zeros((amount,), jnp.int32).at[order[jnp.where(places < fixed, places, moved)]].set(jnp.asarray(sizes, jnp.int32))

    sizes = jnp.where(number % 4 == 0, named(crowded, number // 4), named(ordinary, number - number // 4 - 1))
    mixed = jax.random.permutation(jax.random.fold_in(own, 3), amount)
    donor, taker = mixed[0:amount // 2 * 2:2], mixed[1:amount // 2 * 2:2]
    margin = jnp.minimum(sizes[donor] - 1, limit - sizes[taker]) // 2
    margin = jnp.where((donor == order[0]) | (taker == order[0]) | (sizes[taker] == 0), 0, jnp.maximum(margin, 0))
    moved = jax.random.randint(jax.random.fold_in(own, 4), (amount // 2,), 0, 1 << 20) % (margin + 1)
    sizes = sizes.at[donor].add(-moved).at[taker].add(moved)
    members = jnp.searchsorted(jnp.cumsum(sizes), jnp.arange(rows * top), side="right").astype(jnp.int32)
    table = members.reshape(top, rows).T
    table = table[jax.random.permutation(jax.random.fold_in(own, 1), rows)]
    rotation = jax.random.randint(jax.random.fold_in(own, 2), (rows, 1), 0, top)
    return jnp.take_along_axis(table, (jnp.arange(top)[None, :] + rotation) % top, axis=1)


def portions_of(number_of, total, bound, lean, full):
    loads = [(1 << 20) // math.isqrt(rank ** lean) + 1 for rank in range(1, number_of + 1)]
    largest = bound if full else min(bound, max(-(-total // number_of), total * loads[0] // sum(loads)))
    least = 1 if total - largest >= number_of - 1 else 0
    holding, spare = [largest] + [least] * (number_of - 1), total - largest - least * (number_of - 1)
    while spare > 0:
        free = [i for i in range(1, number_of) if holding[i] < largest] or [i for i in range(1, number_of) if holding[i] < bound]
        pool, remaining = sum([loads[i] for i in free]), spare
        for i in free:
            addition = min(bound - holding[i], max(1, remaining * loads[i] // pool), spare)
            holding[i] = holding[i] + addition
            spare = spare - addition
    return np.array(holding)


def scatter_about(rng, dims, width, reach, pieces=(), kind=jnp.bfloat16):
    loudness = block_scale(rng, dims, pieces, -0.22, 0.18) if pieces else 1.0
    array = jax.random.normal(rng, dims, jnp.float32) * width * loudness
    return jnp.minimum(jnp.maximum(array, -reach), reach).astype(kind)


def setup_inputs(seed: int = 0) -> dict:
    keys = jax.random.split(jax.random.key(seed), 15)
    pool_input = draw_pool_input(jax.random.fold_in(keys[14], 71), 0)
    doc_ids = jnp.searchsorted(jnp.cumsum(uneven_parts(keys[1], DOCS, TOKENS, DOC_MOST, 2)), jnp.arange(TOKENS), side="right").astype(jnp.int32)
    pool_map = scatter_about(keys[2], (GROUPS, GROUP_W, GROUP_W), GROUP_W ** -0.5, 0.5)
    pool_scale = jnp.clip(1.0 + 0.18 * jax.random.normal(keys[3], (POOL_W,), jnp.float32), 0.1, 1.9)
    w_out = scatter_about(keys[4], (POOL_W, D), POOL_W ** -0.5, 0.25)
    residual = scatter_about(keys[5], (TOKENS, D), 1.0, 6.0, ((0, 32),))
    mix_gain = jnp.clip(1.0 + 0.18 * jax.random.normal(keys[6], (D,), jnp.float32), 0.1, 1.9)
    ffn_gain = jnp.clip(1.0 + 0.18 * jax.random.normal(keys[7], (D,), jnp.float32), 0.1, 1.9)
    out_gain = jnp.clip(1.0 + 0.18 * jax.random.normal(keys[8], (D,), jnp.float32), 0.1, 1.9)
    expert_ids_keys = jax.random.split(jax.random.fold_in(keys[9], 1), TOKENS // ROWS_DEV)
    expert_ids_turns = jax.random.permutation(jax.random.fold_in(keys[9], 3), TOKENS // ROWS_DEV)
    expert_ids = jax.vmap(lambda own, number: deal_out(jax.random.fold_in(keys[9], 2), own, number, ROWS_DEV, EXPERTS, TOP_K, CAP, 2))(expert_ids_keys, expert_ids_turns).reshape((TOKENS, TOP_K))
    route_logits = scatter_about(keys[10], (TOKENS, TOP_K), 1.5, 6.0, ((0, 32),), jnp.float32)
    w_gate = scatter_about(keys[11], (EXPERTS, D, FF), D ** -0.5, 0.125, ((0, 32),))
    w_up = scatter_about(keys[12], (EXPERTS, D, FF), D ** -0.5, 0.125, ((0, 32),))
    w_down = scatter_about(keys[13], (EXPERTS, FF, D), FF ** -0.5, 0.1875, ((0, 32),))
    return dict(pool_input=pool_input, doc_ids=doc_ids, pool_map=pool_map, pool_scale=pool_scale, w_out=w_out, residual=residual, mix_gain=mix_gain, ffn_gain=ffn_gain, out_gain=out_gain, expert_ids=expert_ids, route_logits=route_logits, w_gate=w_gate, w_up=w_up, w_down=w_down)


def rms_scale(vector):
    return lax.rsqrt(lax.optimization_barrier(jnp.mean(vector * vector, axis=-1, keepdims=True)) + 1e-06)

def reference(pool_input, doc_ids, pool_map, pool_scale, w_out, residual, mix_gain, ffn_gain, out_gain, expert_ids, route_logits, w_gate, w_up, w_down):
    total_len = doc_ids.shape[0]
    positions = jnp.arange(total_len, dtype=jnp.int32)
    resets = jnp.concatenate([jnp.ones((1,), bool), doc_ids[1:] != doc_ids[:-1]])
    starts = lax.cummax(jnp.where(resets, positions, 0), axis=0).astype(jnp.int32)
    doc_position = (positions - starts + 1).astype(jnp.int32)
    values = pool_input.astype(jnp.float32)
    prefix = jnp.cumsum(values, axis=2)
    before = jnp.concatenate([jnp.zeros(values.shape[:2] + (1,), jnp.float32), prefix[:, :, :-1]], axis=2)
    running = prefix - jnp.take(before, starts, axis=2)
    mean_list = []
    for group_idx in range(GROUPS):
        span_len = TOK_DEV * 2 ** group_idx
        shifted = jnp.pad(running[group_idx], ((0, 0), (span_len, 0)))[:, :total_len]
        counts_in = jnp.minimum(doc_position, span_len).astype(jnp.float32)
        window = running[group_idx] - jnp.where(doc_position > span_len, shifted, jnp.float32(0.0))
        mean_list.append(window / counts_in)
    window_mean = jnp.stack(mean_list)
    pool_diff = (window_mean - values).astype(jnp.bfloat16)
    mapped = jnp.einsum('gct,gcd->tgd', pool_diff.astype(jnp.float32), pool_map.astype(jnp.float32))
    mapped = (mapped.reshape(total_len, -1) * pool_scale).astype(jnp.bfloat16)
    projected = jnp.dot(mapped, w_out, preferred_element_type=jnp.float32)
    stream = (residual.astype(jnp.float32) + mix_gain * projected * rms_scale(projected)).astype(jnp.bfloat16)
    stream_back = stream.astype(jnp.float32)
    normed = (ffn_gain * stream_back * rms_scale(stream_back)).astype(jnp.bfloat16)
    route_weight = jax.nn.sigmoid(route_logits - route_logits[:, ::-1])
    flat_expert = expert_ids.reshape(-1).astype(jnp.int32)
    flat_weight = route_weight.reshape(-1)
    flat_token = (jnp.arange(flat_expert.shape[0], dtype=jnp.int32) // TOP_K).astype(jnp.int32)
    sort_order = jnp.argsort(flat_expert, stable=True).astype(jnp.int32)
    counts = jnp.bincount(flat_expert, length=EXPERTS).astype(jnp.int32)
    expert_starts = (jnp.cumsum(counts) - counts).astype(jnp.int32)
    most_rows = DEVICES * CAP
    order_padded = jnp.concatenate([sort_order, jnp.zeros((most_rows,), jnp.int32)])

    def one_expert(total_y, expert):
        picked = lax.dynamic_slice_in_dim(order_padded, expert_starts[expert], most_rows)
        live_rows = jnp.arange(most_rows, dtype=jnp.int32) < counts[expert]
        tokens = flat_token[picked]
        row_data = normed[tokens]
        gate_act = jnp.dot(row_data, w_gate[expert], preferred_element_type=jnp.float32)
        up_act = jnp.dot(row_data, w_up[expert], preferred_element_type=jnp.float32)
        hidden = (jax.nn.silu(gate_act) * up_act).astype(jnp.bfloat16)
        expert_out = jnp.dot(hidden, w_down[expert], preferred_element_type=jnp.float32).astype(jnp.bfloat16)
        weight = jnp.where(live_rows, flat_weight[picked], jnp.float32(0.0))
        return (total_y.at[tokens].add(expert_out.astype(jnp.float32) * weight[:, None]), None)
    expert_sum, _ = lax.scan(one_expert, jnp.zeros((total_len, normed.shape[1]), jnp.float32), jnp.arange(EXPERTS, dtype=jnp.int32))
    return (stream_back + out_gain * expert_sum * rms_scale(expert_sum)).astype(jnp.bfloat16)
```

```python
import jax
import jax.numpy as jnp
from jax import lax
from jax.sharding import Mesh, PartitionSpec as P

BF16, F32 = jnp.bfloat16, jnp.float32
SP = ("zh", "sl")
HALF = ("sl", "tp")
ALL = ("zh", "sl", "tp")


def to_twin(x):
    return lax.ppermute(x, "zh", [(0, 1), (1, 0)])


def passed_along(x, by):
    devices = lax.axis_size("zh") * lax.axis_size("sl")
    return lax.ppermute(x, SP, [(i, i + by) for i in range(devices - by)])


def rms_scale(vector):
    return lax.rsqrt(jnp.mean(vector * vector, axis=-1, keepdims=True) + 1e-06)


def dot(a, b):
    return jnp.dot(a, b, preferred_element_type=F32)


def dot_t(a, b):
    return lax.dot_general(a, b, (((0,), (0,)), ((), ())), preferred_element_type=F32)


def expert_rows(rows, w_gate, w_up, w_down):
    hidden = (jax.nn.silu(dot(rows, w_gate[0])) * dot(rows, w_up[0])).astype(BF16)
    return dot(hidden, w_down[0]).astype(BF16)


def mixed(mapped, residual, w_out, mix_gain, ffn_gain):
    projected = dot(mapped, w_out)
    stream = residual.astype(F32) + mix_gain * projected * rms_scale(projected)
    stream = lax.reduce_precision(stream, 8, 7)
    return stream, (ffn_gain * stream * rms_scale(stream)).astype(BF16)


def routes(ids, logits, first, experts, capacity):
    rows = ids.shape[1]
    expert = jnp.arange(experts, dtype=F32)[:, None]
    named = [(ids[k : k + 1] - first == expert) for k in range(2)]
    held = (named[0] | named[1]).astype(BF16)
    at = jnp.arange(rows)
    earlier = (at[:, None] < at[None, :]).astype(BF16)
    rank = dot(held, earlier)
    slots = [
        jnp.sum(jnp.where(n, expert * capacity + rank + 1.0, 0.0), axis=0, keepdims=True) - 1.0
        for n in named
    ]
    slot = jnp.arange(experts * capacity, dtype=F32)[:, None]
    hits = [slot == s for s in slots]
    pick = (hits[0] | hits[1]).astype(BF16)
    weights = [
        jax.nn.sigmoid(logits[0:1] - logits[1:2]),
        jax.nn.sigmoid(logits[1:2] - logits[0:1]),
    ]
    weight = jnp.where(hits[0], weights[0], 0.0) + jnp.where(hits[1], weights[1], 0.0)
    high = lax.reduce_precision(weight, 8, 7)
    return pick, high.astype(BF16), (weight - high).astype(BF16)


def local(
    pool_input,
    doc_ids,
    pool_map,
    pool_scale,
    w_out,
    residual,
    mix_gain,
    ffn_gain,
    out_gain,
    expert_ids,
    route_logits,
    w_gate,
    w_up,
    w_down,
):
    groups, channels, length = pool_input.shape
    tp = lax.axis_size("tp")
    blocks = lax.axis_size("zh") * lax.axis_size("sl")
    mine = lax.axis_index(SP)
    rows, width = residual.shape
    experts = w_gate.shape[0] * lax.axis_size("sl") * tp
    capacity = max(2, rows * expert_ids.shape[1] // experts)

    far_blocks = [passed_along(pool_input[g], 2**g) for g in range(groups)]
    far_residual = to_twin(residual)

    flat = pool_input.reshape(groups * channels, length)
    at = jnp.arange(length, dtype=jnp.int32)
    same = doc_ids[:, None] == doc_ids[None, :]
    within = ((at[:, None] <= at[None, :]) & same).astype(BF16)
    tail = (doc_ids == doc_ids[-1])[None, :]
    tail_sums = lax.dot_general(
        tail.astype(BF16), flat, (((1,), (1,)), ((), ())), preferred_element_type=F32
    ).reshape(-1)
    tail_count = jnp.sum(tail.astype(F32))
    meta = jnp.stack([tail_count, doc_ids[-1].astype(F32)])
    ids_t = expert_ids.astype(F32).T
    logits_t = route_logits.T
    parts = [tail_sums, jnp.pad(meta, (0, 126)), ids_t.reshape(-1), logits_t.reshape(-1)]
    sizes = [p.shape[0] for p in parts]
    payload = jnp.concatenate(parts)
    payload = jnp.pad(payload, (0, -payload.shape[0] % 1024)).reshape(-1, 128)
    news = lax.all_to_all(
        jnp.broadcast_to(payload[None], (blocks,) + payload.shape), SP, 0, 0, tiled=True
    )
    news = news.reshape(blocks, -1)
    sums = news[:, : sizes[0]]
    counts = news[:, sizes[0]][:, None]
    lasts = news[:, sizes[0] + 1][:, None]
    block = jnp.arange(blocks, dtype=jnp.int32)[:, None]
    joins = (block < mine) & (lasts == doc_ids[0].astype(F32))
    reach = 2 ** (jnp.arange(groups * channels, dtype=jnp.int32) // channels)[None, :]
    between_on = (block < mine) & (block > mine - reach)
    carry = jnp.sum(jnp.where(joins, sums, 0.0), axis=0)[:, None]
    between = jnp.sum(jnp.where(between_on, sums, 0.0), axis=0)[:, None]
    carry_count = jnp.sum(jnp.where(joins, counts, 0.0))

    local_run = dot(flat, within)
    first_doc = (doc_ids == doc_ids[0])[None, :]
    local_count = jnp.sum(within.astype(F32), axis=0, keepdims=True)
    position = local_count + jnp.where(first_doc, carry_count, 0.0)
    after = (at[:, None] > at[None, :]).astype(BF16)
    far_sum = dot(jnp.concatenate(far_blocks, axis=0), after)
    span = (length * reach.reshape(-1, 1)).astype(F32)
    started = position > span
    window = local_run + jnp.where(
        started, between + far_sum, jnp.where(first_doc, carry, 0.0)
    )
    diff = (window / jnp.minimum(position, span) - flat.astype(F32)).astype(BF16)

    diff = diff.reshape(groups, channels, tp, rows).transpose(2, 0, 1, 3)
    by_row = lax.all_to_all(diff, "tp", 0, 0, tiled=True)
    maps = pool_map.reshape(groups, tp, channels, -1)
    mapped = jnp.concatenate(
        [
            dot_t(by_row[:, g].reshape(tp * channels, rows), maps[g].reshape(tp * channels, -1))
            for g in range(groups)
        ],
        axis=1,
    )
    mapped = (mapped * pool_scale).astype(BF16)
    far_mapped = to_twin(mapped)

    half = lax.axis_index("zh")
    twin = (1 - half) * (blocks // 2) + lax.axis_index("sl")
    first = (half * experts).astype(F32)
    base = sizes[0] + sizes[1]
    twin_news = lax.dynamic_index_in_dim(news, twin, 0, keepdims=False)
    twin_ids = twin_news[base : base + 2 * rows].reshape(2, rows)
    twin_logits = twin_news[base + 2 * rows : base + 4 * rows].reshape(2, rows)
    own_pick, own_high, own_low = routes(ids_t, logits_t, first, experts, capacity)
    far_pick, far_high, far_low = routes(twin_ids, twin_logits, first, experts, capacity)

    def there(send):
        send = send.reshape(experts, capacity, width)
        return lax.all_to_all(send, HALF, 0, 0, tiled=True).reshape(-1, width)

    stream, normed = mixed(mapped, residual, w_out, mix_gain, ffn_gain)
    own_in = there(dot(own_pick, normed).astype(BF16))
    _, far_normed = mixed(far_mapped, far_residual, w_out, mix_gain, ffn_gain)
    far_in = there(dot(far_pick, far_normed).astype(BF16))
    own_out = expert_rows(own_in, w_gate, w_up, w_down)
    far_out = expert_rows(far_in, w_gate, w_up, w_down)
    far_back = there(far_out)
    far_part = (dot_t(far_high, far_back) + dot_t(far_low, far_back)).astype(BF16)
    other_part = to_twin(far_part)
    own_back = there(own_out)
    expert_sum = dot_t(own_high, own_back) + dot_t(own_low, own_back) + other_part.astype(F32)
    return (stream + out_gain * expert_sum * rms_scale(expert_sum)).astype(BF16)


def solution(mesh):
    sp, tp = mesh.shape["sp"], mesh.shape["tp"]
    fine = Mesh(mesh.devices.reshape(2, sp // 2, tp), ALL)
    rowwise = P(ALL, None)
    each = P(ALL, None, None)
    in_specs = (
        P(None, "tp", SP),
        P(SP),
        P(),
        P(),
        P(),
        rowwise,
        P(),
        P(),
        P(),
        rowwise,
        rowwise,
        each,
        each,
        each,
    )
    return jax.shard_map(local, mesh=fine, in_specs=in_specs, out_specs=rowwise, check_vma=False)
```

```python
import functools
import math

import jax
import jax.numpy as jnp
from jax import lax
from jax.experimental import pallas as pl
from jax.experimental.pallas import tpu as pltpu
from jax.sharding import Mesh, PartitionSpec as P


BF16, F32 = jnp.bfloat16, jnp.float32
SP = ("zh", "zl", "yc")
HALF = ("zl", "yc", "tp")
ALL = ("zh", "zl", "yc", "tp")
LANES = 128
PIECES = 3
VM = pl.BlockSpec(memory_space=pltpu.VMEM)
SM = pl.BlockSpec(memory_space=pltpu.SMEM)


def in_hbm(x):
    return pltpu.with_memory_space_constraint(x, pltpu.HBM)


def to_twin(x, inner=True, outer=True):
    last = 2 * lax.axis_size("zl") - 1
    places = range(last + 1)
    used = [i for i in places if (outer if i in (0, last) else inner)]
    return (lax.ppermute(x, ("zh", "zl"), [(i, last - i) for i in used]))


def passed_along(x, by):
    devices = lax.axis_size("zh") * lax.axis_size("zl") * lax.axis_size("yc")
    return (lax.ppermute(x, SP, [(i, i + by) for i in range(devices - by)]))


def rms_scale(vector):
    return lax.rsqrt(jnp.mean(vector * vector, axis=-1, keepdims=True) + 1e-06)


def dot(a, b):
    return jnp.dot(a, b, preferred_element_type=F32)


def dot_t(a, b):
    return lax.dot_general(a, b, (((0,), (0,)), ((), ())), preferred_element_type=F32)


def dot_nt(a, b):
    return lax.dot_general(a, b, (((1,), (1,)), ((), ())), preferred_element_type=F32)


def iota(shape, dim):
    return lax.broadcasted_iota(jnp.int32, shape, dim)


def column(row):
    return jnp.transpose(jnp.broadcast_to(row, (8, row.shape[1])))[:, :1]


def call(kernel, outs, *args, vmem=16 * 2**20, flops=0):
    specs = [SM if a.ndim == 1 else VM for a in args]
    shapes = [(pltpu.HBM if where else jax.ShapeDtypeStruct)(s, d) for s, d, *where in outs]
    moved = sum(a.size * a.dtype.itemsize for a in args)
    moved += sum(math.prod(s) * jnp.dtype(d).itemsize for s, d, *_ in outs)
    return pl.pallas_call(
        kernel,
        out_shape=shapes,
        in_specs=specs,
        out_specs=[VM] * len(shapes),
        compiler_params=pltpu.CompilerParams(vmem_limit_bytes=vmem),
        cost_estimate=pl.CostEstimate(flops=flops, transcendentals=0, bytes_accessed=moved),
    )(*args)


def head_kernel(x_ref, docs_ref, ids_ref, logits_ref, res_ref, news_ref, *refs):
    groups, channels, length = x_ref.shape
    block_refs, piece_refs = refs[:groups], refs[groups:]
    part = piece_refs[0].shape[0]
    piece_refs[0][...] = res_ref[:part]
    piece_refs[1][...] = res_ref[part:]
    piece_refs[2][...] = res_ref[...]
    blocks = news_ref.shape[0]
    docs = docs_ref[...]
    tail = docs == docs[:, length - 1 :]
    flat = x_ref[...].reshape(groups * channels, length)
    tails = jnp.broadcast_to(jnp.where(tail, 1.0, 0.0), (8, length)).astype(BF16)
    sums = dot_nt(tails, flat)[:1]
    count = jnp.sum(jnp.where(tail, 1.0, 0.0), axis=1, keepdims=True)
    wide = (1, LANES)
    lines = [sums[:, i : i + LANES] for i in range(0, groups * channels, LANES)]
    lines.append(jnp.broadcast_to(count, wide))
    lines.append(jnp.broadcast_to(docs[:, length - 1 :].astype(F32), wide))
    rows = ids_ref.shape[1]
    for ref in (ids_ref, logits_ref):
        for k in range(2):
            line = ref[k : k + 1].astype(F32)
            lines += [line[:, i : i + LANES] for i in range(0, rows, LANES)]
    spare = news_ref.shape[1] - len(lines)
    lines.append(jnp.zeros((spare, LANES), F32))
    payload = jnp.concatenate(lines, axis=0)
    for b in range(blocks):
        news_ref[b] = payload
    for g in range(groups):
        block_refs[g][...] = x_ref[g]


def pool_kernel(where_ref, x_ref, docs_ref, news_ref, *refs):
    groups, channels, length = x_ref.shape
    far_refs, out_refs = refs[:groups], refs[groups:]
    tp, rows = len(out_refs), out_refs[0].shape[2]
    mine = where_ref[0]
    width = groups * channels
    lines = width // LANES
    docs = docs_ref[...]
    first_doc = docs == docs[:, :1]
    block = iota((news_ref.shape[0], LANES), 0)
    joins = (block < mine) & (news_ref[:, lines + 1, :] == docs[:, :1].astype(F32))
    earlier = jnp.sum(jnp.where(joins, news_ref[:, lines, :], 0.0), axis=0, keepdims=True)[:, :1]
    carries, betweens = [], []
    for i in range(lines):
        sums = news_ref[:, i, :]
        reach = 1 << ((iota(sums.shape, 1) + i * LANES) // channels)
        inside = (block < mine) & (block > mine - reach)
        carries.append(jnp.sum(jnp.where(joins, sums, 0.0), axis=0, keepdims=True))
        betweens.append(jnp.sum(jnp.where(inside, sums, 0.0), axis=0, keepdims=True))
    carry = column(jnp.concatenate(carries, axis=1))
    between = column(jnp.concatenate(betweens, axis=1))
    down, across = iota((length, length), 0), iota((length, length), 1)
    docs_f = docs.astype(F32)
    within = (down <= across) & (column(docs_f) == docs_f)
    within = jnp.where(within, 1.0, 0.0)
    position = jnp.sum(within, axis=0, keepdims=True) + jnp.where(first_doc, earlier, 0.0)
    within = within.astype(BF16)
    after = jnp.where(down > across, 1.0, 0.0).astype(BF16)
    for g in range(groups):
        x = x_ref[g]
        part = slice(g * channels, (g + 1) * channels)
        span = float(length * 2**g)
        near = dot(x, within)
        far = dot(far_refs[g][...], after)
        begun = jnp.where(first_doc, carry[part], 0.0)
        window = near + jnp.where(position > span, between[part] + far, begun)
        diff = (window / jnp.minimum(position, span) - x.astype(F32)).astype(BF16)
        for j in range(tp):
            for away in range(tp):

                @pl.when(where_ref[3] == (j - away) % tp)
                def _():
                    out_refs[away][g] = diff[:, j * rows : (j + 1) * rows]


def map_kernel(where_ref, maps_ref, scale_ref, *refs):
    d_refs, out_ref = refs[:-1], refs[-1]
    tp, (groups, channels, rows) = len(d_refs), d_refs[0].shape
    wide = maps_ref.shape[2]
    for g in range(groups):
        total = jnp.zeros((rows, wide), F32)
        for away in range(tp):
            source = lax.rem(where_ref[3] + tp - away, tp)
            start = pl.multiple_of(source * channels, channels)
            total += dot_t(d_refs[away][g], maps_ref[g, pl.ds(start, channels)])
        part = slice(g * wide, (g + 1) * wide)
        out_ref[:, part] = (total * scale_ref[:, part]).astype(BF16)


def slots_of(ids, first, experts, capacity):
    rows = ids[0].shape[1]
    expert = iota((experts, rows), 0).astype(F32)
    named = [i - first == expert for i in ids]
    held = jnp.where(named[0] | named[1], 1.0, 0.0).astype(BF16)
    earlier = jnp.where(iota((rows, rows), 0) < iota((rows, rows), 1), 1.0, 0.0).astype(BF16)
    place = dot(held, earlier) + expert * float(capacity) + 1.0
    return [jnp.sum(jnp.where(n, place, 0.0), axis=0, keepdims=True) - 1.0 for n in named]


def read_routes(where_ref, news_ref, skip, rows):
    at, step = where_ref[1], rows // LANES
    out = []
    for k in range(4):
        out.append(
            jnp.concatenate(
                [news_ref[at, pl.ds(skip + k * step + i, 1), :] for i in range(step)], axis=1
            )
        )
    return out[:2], out[2:]


def table_kernel(capacity, skip, where_ref, news_ref, pick_ref, weight_ref):
    slots, rows = pick_ref.shape
    experts = slots // capacity
    ids, logits = read_routes(where_ref, news_ref, skip, rows)
    at = slots_of(ids, where_ref[2].astype(F32), experts, capacity)
    slot = iota((slots, rows), 0).astype(F32)
    pick_ref[...] = jnp.where((slot == at[0]) | (slot == at[1]), 1.0, 0.0).astype(BF16)
    weights = [jax.nn.sigmoid(logits[0] - logits[1]), jax.nn.sigmoid(logits[1] - logits[0])]
    slot = iota((rows, slots), 1).astype(F32)
    weight = jnp.zeros((rows, slots), F32)
    for k in range(2):
        weight = jnp.where(slot == column(at[k]), column(weights[k]), weight)
    weight_ref[...] = weight.astype(BF16)


def send_kernel(where_ref, mapped_ref, w_ref, mix_ref, ffn_ref, pick_ref, *refs):
    n = 1 if refs[0].shape[0] == mapped_ref.shape[0] else PIECES
    res_refs, send_ref, stream_refs = refs[:n], refs[n], refs[n + 1 :]
    projected = dot(mapped_ref[...], w_ref[...])
    residual = res_refs[-1][...]
    if n > 1:
        outer = jnp.concatenate([r[...] for r in res_refs[:-1]], axis=0)
        residual = jnp.where(where_ref[4] == 1, outer, residual)
    stream = residual.astype(F32) + mix_ref[...] * projected * rms_scale(projected)
    stream = stream.astype(BF16)
    if stream_refs:
        stream_refs[0][...] = stream
    stream = stream.astype(F32)
    normed = (ffn_ref[...] * stream * rms_scale(stream)).astype(BF16)
    send_ref[...] = dot(pick_ref[...], normed).astype(BF16)


def sum_kernel(weight_ref, back_ref, out_ref):
    out_ref[...] = dot(weight_ref[...], back_ref[...]).astype(out_ref.dtype)


def last_kernel(own_0, own_1, other_0, other_1, stream_ref, gain_ref, out_ref):
    total = jnp.concatenate(
        [own_0[...] + other_0[...].astype(F32), own_1[...] + other_1[...].astype(F32)], axis=1
    )
    out = stream_ref[...].astype(F32) + gain_ref[...] * total * rms_scale(total)
    out_ref[...] = out.astype(BF16)


def expert_kernel(tiles, x_ref, gate_ref, up_ref, down_ref, *refs):
    out_refs, hidden_ref = refs[:-1], refs[-1]
    step = pl.program_id(0)
    tile = gate_ref.shape[2]

    @pl.when(step < tiles)
    def _():
        x = x_ref[...]
        gate, up = dot(x, gate_ref[0]), dot(x, up_ref[0])
        hidden = (gate / (1.0 + jnp.exp(-gate)) * up).astype(BF16)
        hidden_ref[:, pl.ds(pl.multiple_of(step * tile, tile), tile)] = hidden

    for i, out_ref in enumerate(out_refs):

        @pl.when(step == tiles + i)
        def _():
            out_ref[...] = dot(hidden_ref[...], down_ref[0]).astype(BF16)


def expert_rows(x, w_gate, w_up, w_down, parts, columns):
    n, width = x.shape
    inner = w_gate.shape[2]
    tile = min(inner, 512)
    tiles = inner // tile
    early = lambda i: (0, 0, jnp.minimum(i, tiles - 1))
    whole = lambda i: (0, 0)
    return pl.pallas_call(
        functools.partial(expert_kernel, tiles),
        grid=(tiles + parts,),
        out_shape=[pltpu.HBM((n, columns), BF16)] * parts + [pltpu.HBM((n, inner), BF16)],
        in_specs=[
            pl.BlockSpec((n, width), whole),
            pl.BlockSpec((1, width, tile), early),
            pl.BlockSpec((1, width, tile), early),
            pl.BlockSpec((1, inner, columns), lambda i: (0, 0, jnp.maximum(i - tiles, 0))),
        ],
        out_specs=[pl.BlockSpec((n, columns), whole)] * parts + [pl.BlockSpec((n, inner), whole)],
        compiler_params=pltpu.CompilerParams(
            dimension_semantics=("arbitrary",), vmem_limit_bytes=32 * 2**20
        ),
        cost_estimate=pl.CostEstimate(
            flops=2 * n * inner * (2 * width + parts * columns),
            transcendentals=n * inner,
            bytes_accessed=2 * inner * (2 * width + parts * columns) + 4 * n * width,
        ),
    )(x, w_gate, w_up, w_down)


def down_kernel(hidden_ref, down_ref, out_ref):
    out_ref[...] = dot(hidden_ref[...], down_ref[0]).astype(BF16)


def down_rows(hidden, w_down, start):
    n, inner = hidden.shape
    columns = w_down.shape[2] - start
    tile = min(columns, 1024)
    skip = start // tile
    return pl.pallas_call(
        down_kernel,
        grid=(columns // tile,),
        out_shape=pltpu.HBM((n, columns), BF16),
        in_specs=[
            pl.BlockSpec((n, inner), lambda i: (0, 0)),
            pl.BlockSpec((1, inner, tile), lambda i: (0, 0, i + skip)),
        ],
        out_specs=pl.BlockSpec((n, tile), lambda i: (0, i)),
        compiler_params=pltpu.CompilerParams(vmem_limit_bytes=32 * 2**20),
        cost_estimate=pl.CostEstimate(
            flops=2 * n * inner * columns,
            transcendentals=0,
            bytes_accessed=2 * inner * (columns + n) + 2 * n * columns,
        ),
    )(hidden, w_down)


def local(
    pool_input,
    doc_ids,
    pool_map,
    pool_scale,
    w_out,
    residual,
    mix_gain,
    ffn_gain,
    out_gain,
    expert_ids,
    route_logits,
    *expert_weights,
):
    w_gate, w_up, w_down = [
        pltpu.with_memory_space_constraint(w, pltpu.HBM) for w in expert_weights
    ]
    groups, channels, length = pool_input.shape
    tp, planes, plane = lax.axis_size("tp"), lax.axis_size("zl"), lax.axis_size("yc")
    blocks = 2 * planes * plane
    rows, width = residual.shape
    experts = w_gate.shape[0] * planes * plane * tp
    capacity = max(2, rows * expert_ids.shape[1] // experts)
    slots = experts * capacity
    half, mine = lax.axis_index("zh"), lax.axis_index(SP)
    level = lax.axis_index(("zh", "zl"))
    twin = (2 * planes - 1 - level) * plane + lax.axis_index("yc")
    edge = ((level == 0) | (level == 2 * planes - 1)).astype(jnp.int32)
    first = half * experts
    column_at = lax.axis_index("tp")
    own_at = jnp.stack([mine, mine, first, column_at, edge])
    far_at = jnp.stack([mine, twin, first, column_at, edge])
    docs = in_hbm(doc_ids.reshape(1, length))
    pool_input, residual = in_hbm(pool_input), in_hbm(residual)
    skip = groups * channels // LANES + 2
    lines = skip + 4 * rows // LANES
    lines += -lines % 8
    sizes = (rows // 2, rows // 2, rows)
    news, *own_blocks = call(
        head_kernel,
        [((blocks, lines, LANES), F32)]
        + [((channels, length), BF16)] * groups
        + [((n, width), BF16, True) for n in sizes],
        pool_input,
        docs,
        in_hbm(expert_ids.T),
        in_hbm(route_logits.T),
        residual,
    )
    own_blocks, pieces = own_blocks[:groups], own_blocks[groups:]
    news = (lax.all_to_all(news, SP, 0, 0, tiled=True))
    far_blocks = []
    for g in range(groups):
        far_blocks.append(passed_along(own_blocks[g], 2**g))
    far_pieces = []
    for i in range(PIECES):
        far_pieces.append(to_twin(pieces[i], inner=i == 2, outer=i < 2))
    diffs = call(
        pool_kernel,
        [((groups, channels, rows), BF16)] * tp,
        own_at,
        pool_input,
        docs,
        news,
        *far_blocks,
    )
    diffs = list(diffs)
    for away in range(1, tp):
        turn = [(i, (i + away) % tp) for i in range(tp)]
        diffs[away] = (lax.ppermute(diffs[away], "tp", turn))
    (mapped,) = call(
        map_kernel,
        [((rows, groups * pool_map.shape[2]), BF16)],
        own_at,
        in_hbm(pool_map),
        in_hbm(pool_scale.reshape(1, -1)),
        *diffs,
    )
    far_mapped = to_twin(mapped)
    gains = (in_hbm(mix_gain.reshape(1, -1)), in_hbm(ffn_gain.reshape(1, -1)))
    table = functools.partial(table_kernel, capacity, skip)
    tables = [((slots, rows), BF16), ((rows, slots), BF16, True)]
    own_pick, own_weight = call(table, tables, own_at, news)
    far_pick, far_weight = call(table, tables, far_at, news)

    def there(x):
        columns = x.shape[1]
        x = x.reshape(experts, capacity, columns)
        return (lax.all_to_all(x, HALF, 0, 0, tiled=True).reshape(-1, columns))

    big = 24 * 2**20
    own_send, stream = call(
        send_kernel,
        [((slots, width), BF16, True), ((rows, width), BF16, True)],
        own_at, mapped, w_out, *gains, own_pick, residual,
        vmem=big,
    )
    own_in = there(own_send)
    (far_send,) = call(
        send_kernel,
        [((slots, width), BF16, True)],
        far_at, far_mapped, w_out, *gains, far_pick, *far_pieces,
        vmem=big,
    )
    far_in = there(far_send)
    part = width // 2
    *own_outs, _ = expert_rows(own_in, w_gate, w_up, w_down, 2, part)
    far_out_0, far_hidden = expert_rows(far_in, w_gate, w_up, w_down, 1, part)
    far_out_1 = down_rows(far_hidden, w_down, part)
    others, own_sums = [], []
    for outs in zip((far_out_0, far_out_1), own_outs):
        far_back = there(outs[0])
        (far_part,) = call(
            sum_kernel,
            [((rows, part), BF16)],
            far_weight, far_back,
            vmem=big,
        )
        others.append(to_twin(far_part))
        own_back = there(outs[1])
        own_sums += call(
            sum_kernel,
            [((rows, part), F32)],
            own_weight, own_back,
            vmem=big,
        )
    (out,) = call(
        last_kernel,
        [((rows, width), BF16)],
        *own_sums, *others, stream, in_hbm(out_gain.reshape(1, -1)),
        vmem=big,
    )
    return out


def solution(mesh):
    sp, tp = mesh.shape["sp"], mesh.shape["tp"]
    planes = 2 if sp % 4 == 0 else 1
    fine = Mesh(mesh.devices.reshape(2, planes, sp // (2 * planes), tp), ALL)
    rowwise = P(ALL, None)
    each = P(ALL, None, None)
    in_specs = (
        P(None, "tp", SP),
        P(SP),
        P(),
        P(),
        P(),
        rowwise,
        P(),
        P(),
        P(),
        rowwise,
        rowwise,
        each,
        each,
        each,
    )

    return jax.shard_map(local, mesh=fine, in_specs=in_specs, out_specs=rowwise, check_vma=False)
```

```python
import functools
import math

import jax
import jax.numpy as jnp
from jax import lax
from jax.experimental import pallas as pl
from jax.experimental.pallas import tpu as pltpu
from jax.sharding import Mesh, PartitionSpec as P


BF16, F32 = jnp.bfloat16, jnp.float32
SP = ("zh", "zl", "yc")
HALF = ("zl", "yc", "tp")
ALL = ("zh", "zl", "yc", "tp")
LANES = 128
PIECES = 3
VM = pl.BlockSpec(memory_space=pltpu.VMEM)
SM = pl.BlockSpec(memory_space=pltpu.SMEM)


def in_hbm(x):
    return pltpu.with_memory_space_constraint(x, pltpu.HBM)


def to_twin(x, inner=True, outer=True):
    last = 2 * lax.axis_size("zl") - 1
    places = range(last + 1)
    used = [i for i in places if (outer if i in (0, last) else inner)]
    return (lax.ppermute(x, ("zh", "zl"), [(i, last - i) for i in used]))


def passed_along(x, by):
    devices = lax.axis_size("zh") * lax.axis_size("zl") * lax.axis_size("yc")
    return (lax.ppermute(x, SP, [(i, i + by) for i in range(devices - by)]))


def rms_scale(vector):
    return lax.rsqrt(jnp.mean(vector * vector, axis=-1, keepdims=True) + 1e-06)


def dot(a, b):
    return jnp.dot(a, b, preferred_element_type=F32)


def dot_t(a, b):
    return lax.dot_general(a, b, (((0,), (0,)), ((), ())), preferred_element_type=F32)


def dot_nt(a, b):
    return lax.dot_general(a, b, (((1,), (1,)), ((), ())), preferred_element_type=F32)


def iota(shape, dim):
    return lax.broadcasted_iota(jnp.int32, shape, dim)


def column(row):
    return jnp.transpose(jnp.broadcast_to(row, (8, row.shape[1])))[:, :1]


def call(kernel, outs, *args, vmem=16 * 2**20, flops=0):
    specs = [SM if a.ndim == 1 else VM for a in args]
    shapes = [(pltpu.HBM if where else jax.ShapeDtypeStruct)(s, d) for s, d, *where in outs]
    moved = sum(a.size * a.dtype.itemsize for a in args)
    moved += sum(math.prod(s) * jnp.dtype(d).itemsize for s, d, *_ in outs)
    return pl.pallas_call(
        kernel,
        out_shape=shapes,
        in_specs=specs,
        out_specs=[VM] * len(shapes),
        compiler_params=pltpu.CompilerParams(vmem_limit_bytes=vmem),
        cost_estimate=pl.CostEstimate(flops=flops, transcendentals=0, bytes_accessed=moved),
    )(*args)


def head_kernel(x_ref, docs_ref, ids_ref, logits_ref, res_ref, news_ref, *refs):
    groups, channels, length = x_ref.shape
    block_refs, piece_refs = refs[:groups], refs[groups:]
    part = piece_refs[0].shape[0]
    piece_refs[0][...] = res_ref[:part]
    piece_refs[1][...] = res_ref[part:]
    blocks = news_ref.shape[0]
    docs = docs_ref[...]
    tail = docs == docs[:, length - 1 :]
    flat = x_ref[...].reshape(groups * channels, length)
    tails = jnp.broadcast_to(jnp.where(tail, 1.0, 0.0), (8, length)).astype(BF16)
    sums = dot_nt(tails, flat)[:1]
    count = jnp.sum(jnp.where(tail, 1.0, 0.0), axis=1, keepdims=True)
    wide = (1, LANES)
    lines = [sums[:, i : i + LANES] for i in range(0, groups * channels, LANES)]
    lines.append(jnp.broadcast_to(count, wide))
    lines.append(jnp.broadcast_to(docs[:, length - 1 :].astype(F32), wide))
    rows = ids_ref.shape[1]
    for ref in (ids_ref, logits_ref):
        for k in range(2):
            line = ref[k : k + 1].astype(F32)
            lines += [line[:, i : i + LANES] for i in range(0, rows, LANES)]
    spare = news_ref.shape[1] - len(lines)
    lines.append(jnp.zeros((spare, LANES), F32))
    payload = jnp.concatenate(lines, axis=0)
    for b in range(blocks):
        news_ref[b] = payload
    for g in range(groups):
        block_refs[g][...] = x_ref[g]


def pool_kernel(where_ref, x_ref, docs_ref, news_ref, *refs):
    groups, channels, length = x_ref.shape
    far_refs, out_refs = refs[:groups], refs[groups:]
    tp, rows = len(out_refs), out_refs[0].shape[2]
    mine = where_ref[0]
    width = groups * channels
    lines = width // LANES
    docs = docs_ref[...]
    first_doc = docs == docs[:, :1]
    block = iota((news_ref.shape[0], LANES), 0)
    joins = (block < mine) & (news_ref[:, lines + 1, :] == docs[:, :1].astype(F32))
    earlier = jnp.sum(jnp.where(joins, news_ref[:, lines, :], 0.0), axis=0, keepdims=True)[:, :1]
    carries, betweens = [], []
    for i in range(lines):
        sums = news_ref[:, i, :]
        reach = 1 << ((iota(sums.shape, 1) + i * LANES) // channels)
        inside = (block < mine) & (block > mine - reach)
        carries.append(jnp.sum(jnp.where(joins, sums, 0.0), axis=0, keepdims=True))
        betweens.append(jnp.sum(jnp.where(inside, sums, 0.0), axis=0, keepdims=True))
    carry = column(jnp.concatenate(carries, axis=1))
    between = column(jnp.concatenate(betweens, axis=1))
    down, across = iota((length, length), 0), iota((length, length), 1)
    docs_f = docs.astype(F32)
    within = (down <= across) & (column(docs_f) == docs_f)
    within = jnp.where(within, 1.0, 0.0)
    position = jnp.sum(within, axis=0, keepdims=True) + jnp.where(first_doc, earlier, 0.0)
    within = within.astype(BF16)
    after = jnp.where(down > across, 1.0, 0.0).astype(BF16)
    for g in range(groups):
        x = x_ref[g]
        part = slice(g * channels, (g + 1) * channels)
        span = float(length * 2**g)
        near = dot(x, within)
        far = dot(far_refs[g][...], after)
        begun = jnp.where(first_doc, carry[part], 0.0)
        window = near + jnp.where(position > span, between[part] + far, begun)
        diff = (window / jnp.minimum(position, span) - x.astype(F32)).astype(BF16)
        for j in range(tp):
            for away in range(tp):

                @pl.when(where_ref[3] == (j - away) % tp)
                def _():
                    out_refs[away][g] = diff[:, j * rows : (j + 1) * rows]


def map_kernel(where_ref, maps_ref, scale_ref, *refs):
    d_refs, out_ref = refs[:-1], refs[-1]
    tp, (groups, channels, rows) = len(d_refs), d_refs[0].shape
    wide = maps_ref.shape[2]
    for g in range(groups):
        total = jnp.zeros((rows, wide), F32)
        for away in range(tp):
            source = lax.rem(where_ref[3] + tp - away, tp)
            start = pl.multiple_of(source * channels, channels)
            total += dot_t(d_refs[away][g], maps_ref[g, pl.ds(start, channels)])
        part = slice(g * wide, (g + 1) * wide)
        out_ref[:, part] = (total * scale_ref[:, part]).astype(BF16)


def slots_of(ids, first, experts, capacity):
    rows = ids[0].shape[1]
    expert = iota((experts, rows), 0).astype(F32)
    named = [i - first == expert for i in ids]
    held = jnp.where(named[0] | named[1], 1.0, 0.0).astype(BF16)
    earlier = jnp.where(iota((rows, rows), 0) < iota((rows, rows), 1), 1.0, 0.0).astype(BF16)
    place = dot(held, earlier) + expert * float(capacity) + 1.0
    return [jnp.sum(jnp.where(n, place, 0.0), axis=0, keepdims=True) - 1.0 for n in named]


def read_routes(where_ref, news_ref, skip, rows):
    at, step = where_ref[1], rows // LANES
    out = []
    for k in range(4):
        out.append(
            jnp.concatenate(
                [news_ref[at, pl.ds(skip + k * step + i, 1), :] for i in range(step)], axis=1
            )
        )
    return out[:2], out[2:]


def table_kernel(capacity, skip, where_ref, news_ref, pick_ref, weight_ref):
    slots, rows = pick_ref.shape
    experts = slots // capacity
    ids, logits = read_routes(where_ref, news_ref, skip, rows)
    at = slots_of(ids, where_ref[2].astype(F32), experts, capacity)
    slot = iota((slots, rows), 0).astype(F32)
    pick_ref[...] = jnp.where((slot == at[0]) | (slot == at[1]), 1.0, 0.0).astype(BF16)
    weights = [jax.nn.sigmoid(logits[0] - logits[1]), jax.nn.sigmoid(logits[1] - logits[0])]
    slot = iota((rows, slots), 1).astype(F32)
    weight = jnp.zeros((rows, slots), F32)
    for k in range(2):
        weight = jnp.where(slot == column(at[k]), column(weights[k]), weight)
    weight_ref[...] = weight.astype(BF16)


def send_kernel(where_ref, mapped_ref, w_ref, mix_ref, ffn_ref, pick_ref, *refs):
    n = 1 if refs[0].shape[0] == mapped_ref.shape[0] else PIECES
    res_refs, send_ref, stream_refs = refs[:n], refs[n], refs[n + 1 :]
    projected = dot(mapped_ref[...], w_ref[...])
    residual = res_refs[-1][...]
    if n > 1:
        outer = jnp.concatenate([r[...] for r in res_refs[:-1]], axis=0)
        residual = jnp.where(where_ref[4] == 1, outer, residual)
    stream = residual.astype(F32) + mix_ref[...] * projected * rms_scale(projected)
    stream = stream.astype(BF16)
    if stream_refs:
        stream_refs[0][...] = stream
    stream = stream.astype(F32)
    normed = (ffn_ref[...] * stream * rms_scale(stream)).astype(BF16)
    send_ref[...] = dot(pick_ref[...], normed).astype(BF16)


def sum_kernel(weight_ref, back_ref, out_ref):
    out_ref[...] = dot(weight_ref[...], back_ref[...]).astype(out_ref.dtype)


def last_kernel(own_0, own_1, other_0, other_1, stream_ref, gain_ref, out_ref):
    total = jnp.concatenate(
        [own_0[...] + other_0[...].astype(F32), own_1[...] + other_1[...].astype(F32)], axis=1
    )
    out = stream_ref[...].astype(F32) + gain_ref[...] * total * rms_scale(total)
    out_ref[...] = out.astype(BF16)


def expert_kernel(tiles, x_ref, gate_ref, up_ref, down_ref, *refs):
    out_refs, hidden_ref = refs[:-1], refs[-1]
    step = pl.program_id(0)
    tile = gate_ref.shape[2]

    @pl.when(step < tiles)
    def _():
        x = x_ref[...]
        gate, up = dot(x, gate_ref[0]), dot(x, up_ref[0])
        hidden = (gate / (1.0 + jnp.exp(-gate)) * up).astype(BF16)
        hidden_ref[:, pl.ds(pl.multiple_of(step * tile, tile), tile)] = hidden

    for i, out_ref in enumerate(out_refs):

        @pl.when(step == tiles + i)
        def _():
            out_ref[...] = dot(hidden_ref[...], down_ref[0]).astype(BF16)


def expert_rows(x, w_gate, w_up, w_down, parts, columns):
    n, width = x.shape
    inner = w_gate.shape[2]
    tile = min(inner, 512)
    tiles = inner // tile
    early = lambda i: (0, 0, jnp.minimum(i, tiles - 1))
    whole = lambda i: (0, 0)
    return pl.pallas_call(
        functools.partial(expert_kernel, tiles),
        grid=(tiles + parts,),
        out_shape=[pltpu.HBM((n, columns), BF16)] * parts + [pltpu.HBM((n, inner), BF16)],
        in_specs=[
            pl.BlockSpec((n, width), whole),
            pl.BlockSpec((1, width, tile), early),
            pl.BlockSpec((1, width, tile), early),
            pl.BlockSpec((1, inner, columns), lambda i: (0, 0, jnp.maximum(i - tiles, 0))),
        ],
        out_specs=[pl.BlockSpec((n, columns), whole)] * parts + [pl.BlockSpec((n, inner), whole)],
        compiler_params=pltpu.CompilerParams(
            dimension_semantics=("arbitrary",), vmem_limit_bytes=32 * 2**20
        ),
        cost_estimate=pl.CostEstimate(
            flops=2 * n * inner * (2 * width + parts * columns),
            transcendentals=n * inner,
            bytes_accessed=2 * inner * (2 * width + parts * columns) + 4 * n * width,
        ),
    )(x, w_gate, w_up, w_down)


def down_kernel(hidden_ref, down_ref, out_ref):
    out_ref[...] = dot(hidden_ref[...], down_ref[0]).astype(BF16)


def down_rows(hidden, w_down, start):
    n, inner = hidden.shape
    columns = w_down.shape[2] - start
    tile = min(columns, 1024)
    skip = start // tile
    return pl.pallas_call(
        down_kernel,
        grid=(columns // tile,),
        out_shape=pltpu.HBM((n, columns), BF16),
        in_specs=[
            pl.BlockSpec((n, inner), lambda i: (0, 0)),
            pl.BlockSpec((1, inner, tile), lambda i: (0, 0, i + skip)),
        ],
        out_specs=pl.BlockSpec((n, tile), lambda i: (0, i)),
        compiler_params=pltpu.CompilerParams(vmem_limit_bytes=32 * 2**20),
        cost_estimate=pl.CostEstimate(
            flops=2 * n * inner * columns,
            transcendentals=0,
            bytes_accessed=2 * inner * (columns + n) + 2 * n * columns,
        ),
    )(hidden, w_down)


def local(
    pool_input,
    doc_ids,
    pool_map,
    pool_scale,
    w_out,
    residual,
    mix_gain,
    ffn_gain,
    out_gain,
    expert_ids,
    route_logits,
    *expert_weights,
):
    w_gate, w_up, w_down = [
        pltpu.with_memory_space_constraint(w, pltpu.HBM) for w in expert_weights
    ]
    groups, channels, length = pool_input.shape
    tp, planes, plane = lax.axis_size("tp"), lax.axis_size("zl"), lax.axis_size("yc")
    blocks = 2 * planes * plane
    rows, width = residual.shape
    experts = w_gate.shape[0] * planes * plane * tp
    capacity = max(2, rows * expert_ids.shape[1] // experts)
    slots = experts * capacity
    half, mine = lax.axis_index("zh"), lax.axis_index(SP)
    level = lax.axis_index(("zh", "zl"))
    twin = (2 * planes - 1 - level) * plane + lax.axis_index("yc")
    edge = ((level == 0) | (level == 2 * planes - 1)).astype(jnp.int32)
    first = half * experts
    column_at = lax.axis_index("tp")
    own_at = jnp.stack([mine, mine, first, column_at, edge])
    far_at = jnp.stack([mine, twin, first, column_at, edge])
    docs = in_hbm(doc_ids.reshape(1, length))
    residual_in = residual
    pool_input, residual = in_hbm(pool_input), in_hbm(residual)
    skip = groups * channels // LANES + 2
    lines = skip + 4 * rows // LANES
    lines += -lines % 8
    sizes = (rows // 2, rows // 2)
    news, *own_blocks = call(
        head_kernel,
        [((blocks, lines, LANES), F32)]
        + [((channels, length), BF16)] * groups
        + [((n, width), BF16, True) for n in sizes],
        pool_input,
        docs,
        in_hbm(expert_ids.T),
        in_hbm(route_logits.T),
        residual,
    )
    own_blocks, pieces = own_blocks[:groups], [*own_blocks[groups:], residual_in]
    news = (lax.all_to_all(news, SP, 0, 0, tiled=True))
    far_blocks = []
    for g in range(groups):
        far_blocks.append(passed_along(own_blocks[g], 2**g))
    far_pieces = []
    for i in range(PIECES):
        far_pieces.append(to_twin(pieces[i], inner=i == 2, outer=i < 2))
    diffs = call(
        pool_kernel,
        [((groups, channels, rows), BF16)] * tp,
        own_at,
        pool_input,
        docs,
        news,
        *far_blocks,
    )
    diffs = list(diffs)
    for away in range(1, tp):
        turn = [(i, (i + away) % tp) for i in range(tp)]
        diffs[away] = (lax.ppermute(diffs[away], "tp", turn))
    (mapped,) = call(
        map_kernel,
        [((rows, groups * pool_map.shape[2]), BF16)],
        own_at,
        in_hbm(pool_map),
        in_hbm(pool_scale.reshape(1, -1)),
        *diffs,
    )
    far_mapped = to_twin(mapped)
    gains = (in_hbm(mix_gain.reshape(1, -1)), in_hbm(ffn_gain.reshape(1, -1)))
    table = functools.partial(table_kernel, capacity, skip)
    tables = [((slots, rows), BF16), ((rows, slots), BF16, True)]
    own_pick, own_weight = call(table, tables, own_at, news)
    far_pick, far_weight = call(table, tables, far_at, news)

    def there(x):
        columns = x.shape[1]
        x = x.reshape(experts, capacity, columns)
        return (lax.all_to_all(x, HALF, 0, 0, tiled=True).reshape(-1, columns))

    big = 24 * 2**20
    own_send, stream = call(
        send_kernel,
        [((slots, width), BF16, True), ((rows, width), BF16, True)],
        own_at, mapped, w_out, *gains, own_pick, residual,
        vmem=big,
    )
    own_in = there(own_send)
    (far_send,) = call(
        send_kernel,
        [((slots, width), BF16, True)],
        far_at, far_mapped, w_out, *gains, far_pick, *far_pieces,
        vmem=big,
    )
    far_in = there(far_send)
    part = width // 2
    *own_outs, _ = expert_rows(own_in, w_gate, w_up, w_down, 2, part)
    far_out_0, far_hidden = expert_rows(far_in, w_gate, w_up, w_down, 1, part)
    far_out_1 = down_rows(far_hidden, w_down, part)
    others, own_sums = [], []
    for outs in zip((far_out_0, far_out_1), own_outs):
        far_back = there(outs[0])
        (far_part,) = call(
            sum_kernel,
            [((rows, part), BF16)],
            far_weight, far_back,
            vmem=big,
        )
        others.append(to_twin(far_part))
        own_back = there(outs[1])
        own_sums += call(
            sum_kernel,
            [((rows, part), F32)],
            own_weight, own_back,
            vmem=big,
        )
    (out,) = call(
        last_kernel,
        [((rows, width), BF16)],
        *own_sums, *others, stream, in_hbm(out_gain.reshape(1, -1)),
        vmem=big,
    )
    return out


def solution(mesh):
    sp, tp = mesh.shape["sp"], mesh.shape["tp"]
    planes = 2 if sp % 4 == 0 else 1
    fine = Mesh(mesh.devices.reshape(2, planes, sp // (2 * planes), tp), ALL)
    rowwise = P(ALL, None)
    each = P(ALL, None, None)
    in_specs = (
        P(None, "tp", SP),
        P(SP),
        P(),
        P(),
        P(),
        rowwise,
        P(),
        P(),
        P(),
        rowwise,
        rowwise,
        each,
        each,
        each,
    )

    return jax.shard_map(local, mesh=fine, in_specs=in_specs, out_specs=rowwise, check_vma=False)
```

```python
import functools
import math

import jax
import jax.numpy as jnp
from jax import lax
from jax.experimental import pallas as pl
from jax.experimental.pallas import tpu as pltpu
from jax.sharding import Mesh, PartitionSpec as P


BF16, F32 = jnp.bfloat16, jnp.float32
SP = ("zh", "zl", "yc")
HALF = ("zl", "yc", "tp")
ALL = ("zh", "zl", "yc", "tp")
LANES = 128
PIECES = 3
VM = pl.BlockSpec(memory_space=pltpu.VMEM)
SM = pl.BlockSpec(memory_space=pltpu.SMEM)


def in_hbm(x):
    return pltpu.with_memory_space_constraint(x, pltpu.HBM)


def to_twin(x, inner=True, outer=True):
    last = 2 * lax.axis_size("zl") - 1
    places = range(last + 1)
    used = [i for i in places if (outer if i in (0, last) else inner)]
    return (lax.ppermute(x, ("zh", "zl"), [(i, last - i) for i in used]))


def passed_along(x, by):
    devices = lax.axis_size("zh") * lax.axis_size("zl") * lax.axis_size("yc")
    return (lax.ppermute(x, SP, [(i, i + by) for i in range(devices - by)]))


def rms_scale(vector):
    return lax.rsqrt(jnp.mean(vector * vector, axis=-1, keepdims=True) + 1e-06)


def dot(a, b):
    return jnp.dot(a, b, preferred_element_type=F32)


def dot_t(a, b):
    return lax.dot_general(a, b, (((0,), (0,)), ((), ())), preferred_element_type=F32)


def dot_nt(a, b):
    return lax.dot_general(a, b, (((1,), (1,)), ((), ())), preferred_element_type=F32)


def iota(shape, dim):
    return lax.broadcasted_iota(jnp.int32, shape, dim)


def column(row):
    return jnp.transpose(jnp.broadcast_to(row, (8, row.shape[1])))[:, :1]


def call(kernel, outs, *args, vmem=16 * 2**20, flops=0):
    specs = [SM if a.ndim == 1 else VM for a in args]
    shapes = [(pltpu.HBM if where else jax.ShapeDtypeStruct)(s, d) for s, d, *where in outs]
    moved = sum(a.size * a.dtype.itemsize for a in args)
    moved += sum(math.prod(s) * jnp.dtype(d).itemsize for s, d, *_ in outs)
    return pl.pallas_call(
        kernel,
        out_shape=shapes,
        in_specs=specs,
        out_specs=[VM] * len(shapes),
        compiler_params=pltpu.CompilerParams(vmem_limit_bytes=vmem),
        cost_estimate=pl.CostEstimate(flops=flops, transcendentals=0, bytes_accessed=moved),
    )(*args)


def head_kernel(x_ref, docs_ref, ids_ref, logits_ref, res_ref, news_ref, *refs):
    groups, channels, length = x_ref.shape
    block_refs, piece_refs = refs[:groups], refs[groups:]
    part = piece_refs[0].shape[0]
    piece_refs[0][...] = res_ref[:part]
    piece_refs[1][...] = res_ref[part:]
    blocks = news_ref.shape[0]
    docs = docs_ref[...]
    tail = docs == docs[:, length - 1 :]
    flat = x_ref[...].reshape(groups * channels, length)
    tails = jnp.broadcast_to(jnp.where(tail, 1.0, 0.0), (8, length)).astype(BF16)
    sums = dot_nt(tails, flat)[:1]
    count = jnp.sum(jnp.where(tail, 1.0, 0.0), axis=1, keepdims=True)
    wide = (1, LANES)
    lines = [sums[:, i : i + LANES] for i in range(0, groups * channels, LANES)]
    lines.append(jnp.broadcast_to(count, wide))
    lines.append(jnp.broadcast_to(docs[:, length - 1 :].astype(F32), wide))
    rows = ids_ref.shape[1]
    for ref in (ids_ref, logits_ref):
        for k in range(2):
            line = ref[k : k + 1].astype(F32)
            lines += [line[:, i : i + LANES] for i in range(0, rows, LANES)]
    spare = news_ref.shape[1] - len(lines)
    lines.append(jnp.zeros((spare, LANES), F32))
    payload = jnp.concatenate(lines, axis=0)
    for b in range(blocks):
        news_ref[b] = payload
    for g in range(groups):
        block_refs[g][...] = x_ref[g]


def pool_kernel(where_ref, x_ref, docs_ref, news_ref, *refs):
    groups, channels, length = x_ref.shape
    far_refs, out_refs = refs[:groups], refs[groups:]
    tp, rows = len(out_refs), out_refs[0].shape[2]
    mine = where_ref[0]
    width = groups * channels
    lines = width // LANES
    docs = docs_ref[...]
    first_doc = docs == docs[:, :1]
    block = iota((news_ref.shape[0], LANES), 0)
    joins = (block < mine) & (news_ref[:, lines + 1, :] == docs[:, :1].astype(F32))
    earlier = jnp.sum(jnp.where(joins, news_ref[:, lines, :], 0.0), axis=0, keepdims=True)[:, :1]
    carries, betweens = [], []
    for i in range(lines):
        sums = news_ref[:, i, :]
        reach = 1 << ((iota(sums.shape, 1) + i * LANES) // channels)
        inside = (block < mine) & (block > mine - reach)
        carries.append(jnp.sum(jnp.where(joins, sums, 0.0), axis=0, keepdims=True))
        betweens.append(jnp.sum(jnp.where(inside, sums, 0.0), axis=0, keepdims=True))
    carry = column(jnp.concatenate(carries, axis=1))
    between = column(jnp.concatenate(betweens, axis=1))
    down, across = iota((length, length), 0), iota((length, length), 1)
    docs_f = docs.astype(F32)
    within = (down <= across) & (column(docs_f) == docs_f)
    within = jnp.where(within, 1.0, 0.0)
    position = jnp.sum(within, axis=0, keepdims=True) + jnp.where(first_doc, earlier, 0.0)
    within = within.astype(BF16)
    after = jnp.where(down > across, 1.0, 0.0).astype(BF16)
    for g in range(groups):
        x = x_ref[g]
        part = slice(g * channels, (g + 1) * channels)
        span = float(length * 2**g)
        near = dot(x, within)
        far = dot(far_refs[g][...], after)
        begun = jnp.where(first_doc, carry[part], 0.0)
        window = near + jnp.where(position > span, between[part] + far, begun)
        diff = (window / jnp.minimum(position, span) - x.astype(F32)).astype(BF16)
        for j in range(tp):
            for away in range(tp):

                @pl.when(where_ref[3] == (j - away) % tp)
                def _():
                    out_refs[away][g] = diff[:, j * rows : (j + 1) * rows]


def map_kernel(where_ref, maps_ref, scale_ref, *refs):
    d_refs, out_ref = refs[:-1], refs[-1]
    tp, (groups, channels, rows) = len(d_refs), d_refs[0].shape
    wide = maps_ref.shape[2]
    for g in range(groups):
        total = jnp.zeros((rows, wide), F32)
        for away in range(tp):
            source = lax.rem(where_ref[3] + tp - away, tp)
            start = pl.multiple_of(source * channels, channels)
            total += dot_t(d_refs[away][g], maps_ref[g, pl.ds(start, channels)])
        part = slice(g * wide, (g + 1) * wide)
        out_ref[:, part] = (total * scale_ref[:, part]).astype(BF16)


def slots_of(ids, first, experts, capacity):
    rows = ids[0].shape[1]
    expert = iota((experts, rows), 0).astype(F32)
    named = [i - first == expert for i in ids]
    held = jnp.where(named[0] | named[1], 1.0, 0.0).astype(BF16)
    earlier = jnp.where(iota((rows, rows), 0) < iota((rows, rows), 1), 1.0, 0.0).astype(BF16)
    place = dot(held, earlier) + expert * float(capacity) + 1.0
    return [jnp.sum(jnp.where(n, place, 0.0), axis=0, keepdims=True) - 1.0 for n in named]


def read_routes(where_ref, news_ref, skip, rows):
    at, step = where_ref[1], rows // LANES
    out = []
    for k in range(4):
        out.append(
            jnp.concatenate(
                [news_ref[at, pl.ds(skip + k * step + i, 1), :] for i in range(step)], axis=1
            )
        )
    return out[:2], out[2:]


def table_kernel(capacity, skip, where_ref, news_ref, pick_ref, weight_ref):
    slots, rows = pick_ref.shape
    experts = slots // capacity
    ids, logits = read_routes(where_ref, news_ref, skip, rows)
    at = slots_of(ids, where_ref[2].astype(F32), experts, capacity)
    slot = iota((slots, rows), 0).astype(F32)
    pick_ref[...] = jnp.where((slot == at[0]) | (slot == at[1]), 1.0, 0.0).astype(BF16)
    weights = [jax.nn.sigmoid(logits[0] - logits[1]), jax.nn.sigmoid(logits[1] - logits[0])]
    slot = iota((rows, slots), 1).astype(F32)
    weight = jnp.zeros((rows, slots), F32)
    for k in range(2):
        weight = jnp.where(slot == column(at[k]), column(weights[k]), weight)
    weight_ref[...] = weight.astype(BF16)


def send_kernel(where_ref, mapped_ref, w_ref, mix_ref, ffn_ref, pick_ref, *refs):
    n = 1 if refs[0].shape[0] == mapped_ref.shape[0] else PIECES
    res_refs, send_ref, stream_refs = refs[:n], refs[n], refs[n + 1 :]
    projected = dot(mapped_ref[...], w_ref[...])
    residual = res_refs[-1][...]
    if n > 1:
        outer = jnp.concatenate([r[...] for r in res_refs[:-1]], axis=0)
        residual = jnp.where(where_ref[4] == 1, outer, residual)
    stream = residual.astype(F32) + mix_ref[...] * projected * rms_scale(projected)
    stream = stream.astype(BF16)
    if stream_refs:
        stream_refs[0][...] = stream
    stream = stream.astype(F32)
    normed = (ffn_ref[...] * stream * rms_scale(stream)).astype(BF16)
    send_ref[...] = dot(pick_ref[...], normed).astype(BF16)


def sum_kernel(weight_ref, back_ref, out_ref):
    out_ref[...] = dot(weight_ref[...], back_ref[...]).astype(out_ref.dtype)


def last_kernel(own_0, own_1, other_0, other_1, stream_ref, gain_ref, out_ref):
    total = jnp.concatenate(
        [own_0[...] + other_0[...].astype(F32), own_1[...] + other_1[...].astype(F32)], axis=1
    )
    out = stream_ref[...].astype(F32) + gain_ref[...] * total * rms_scale(total)
    out_ref[...] = out.astype(BF16)


def expert_kernel(tiles, x_ref, gate_ref, up_ref, down_ref, *refs):
    out_refs, hidden_ref = refs[:-1], refs[-1]
    step = pl.program_id(0)
    tile = gate_ref.shape[2]

    @pl.when(step < tiles)
    def _():
        x = x_ref[...]
        gate, up = dot(x, gate_ref[0]), dot(x, up_ref[0])
        hidden = (gate / (1.0 + jnp.exp(-gate)) * up).astype(BF16)
        hidden_ref[:, pl.ds(pl.multiple_of(step * tile, tile), tile)] = hidden

    for i, out_ref in enumerate(out_refs):

        @pl.when(step == tiles + i)
        def _():
            out_ref[...] = dot(hidden_ref[...], down_ref[0]).astype(BF16)


def expert_rows(x, w_gate, w_up, w_down, parts, columns):
    n, width = x.shape
    inner = w_gate.shape[2]
    tile = min(inner, 512)
    tiles = inner // tile
    early = lambda i: (0, 0, jnp.minimum(i, tiles - 1))
    whole = lambda i: (0, 0)
    return pl.pallas_call(
        functools.partial(expert_kernel, tiles),
        grid=(tiles + parts,),
        out_shape=[pltpu.HBM((n, columns), BF16)] * parts + [pltpu.HBM((n, inner), BF16)],
        in_specs=[
            pl.BlockSpec((n, width), whole),
            pl.BlockSpec((1, width, tile), early),
            pl.BlockSpec((1, width, tile), early),
            pl.BlockSpec((1, inner, columns), lambda i: (0, 0, jnp.maximum(i - tiles, 0))),
        ],
        out_specs=[pl.BlockSpec((n, columns), whole)] * parts + [pl.BlockSpec((n, inner), whole)],
        compiler_params=pltpu.CompilerParams(
            dimension_semantics=("arbitrary",), vmem_limit_bytes=32 * 2**20
        ),
        cost_estimate=pl.CostEstimate(
            flops=2 * n * inner * (2 * width + parts * columns),
            transcendentals=n * inner,
            bytes_accessed=2 * inner * (2 * width + parts * columns) + 4 * n * width,
        ),
    )(x, w_gate, w_up, w_down)


def down_kernel(hidden_ref, down_ref, out_ref):
    out_ref[...] = dot(hidden_ref[...], down_ref[0]).astype(BF16)


def down_rows(hidden, w_down, start):
    n, inner = hidden.shape
    columns = w_down.shape[2] - start
    tile = min(columns, 1024)
    skip = start // tile
    return pl.pallas_call(
        down_kernel,
        grid=(columns // tile,),
        out_shape=pltpu.HBM((n, columns), BF16),
        in_specs=[
            pl.BlockSpec((n, inner), lambda i: (0, 0)),
            pl.BlockSpec((1, inner, tile), lambda i: (0, 0, i + skip)),
        ],
        out_specs=pl.BlockSpec((n, tile), lambda i: (0, i)),
        compiler_params=pltpu.CompilerParams(vmem_limit_bytes=32 * 2**20),
        cost_estimate=pl.CostEstimate(
            flops=2 * n * inner * columns,
            transcendentals=0,
            bytes_accessed=2 * inner * (columns + n) + 2 * n * columns,
        ),
    )(hidden, w_down)


def local(
    pool_input,
    doc_ids,
    pool_map,
    pool_scale,
    w_out,
    residual,
    mix_gain,
    ffn_gain,
    out_gain,
    expert_ids,
    route_logits,
    *expert_weights,
):
    w_gate, w_up, w_down = [
        pltpu.with_memory_space_constraint(w, pltpu.HBM) for w in expert_weights
    ]
    groups, channels, length = pool_input.shape
    tp, planes, plane = lax.axis_size("tp"), lax.axis_size("zl"), lax.axis_size("yc")
    blocks = 2 * planes * plane
    rows, width = residual.shape
    experts = w_gate.shape[0] * planes * plane * tp
    capacity = max(2, rows * expert_ids.shape[1] // experts)
    slots = experts * capacity
    half, mine = lax.axis_index("zh"), lax.axis_index(SP)
    level = lax.axis_index(("zh", "zl"))
    twin = (2 * planes - 1 - level) * plane + lax.axis_index("yc")
    edge = ((level == 0) | (level == 2 * planes - 1)).astype(jnp.int32)
    first = half * experts
    column_at = lax.axis_index("tp")
    own_at = jnp.stack([mine, mine, first, column_at, edge])
    far_at = jnp.stack([mine, twin, first, column_at, edge])
    docs = in_hbm(doc_ids.reshape(1, length))
    residual_in = residual
    pool_input, residual = in_hbm(pool_input), in_hbm(residual)
    skip = groups * channels // LANES + 2
    lines = skip + 4 * rows // LANES
    lines += -lines % 8
    sizes = (rows // 2, rows // 2)
    news, *own_blocks = call(
        head_kernel,
        [((blocks, lines, LANES), F32)]
        + [((channels, length), BF16)] * groups
        + [((n, width), BF16, True) for n in sizes],
        pool_input,
        docs,
        in_hbm(expert_ids.T),
        in_hbm(route_logits.T),
        residual,
    )
    own_blocks, pieces = own_blocks[:groups], [*own_blocks[groups:], residual_in]
    news = (lax.all_to_all(news, SP, 0, 0, tiled=True))
    far_blocks = []
    for g in range(groups):
        far_blocks.append(passed_along(own_blocks[g], 2**g))
    far_pieces = []
    for i in range(PIECES):
        far_pieces.append(to_twin(pieces[i], inner=i == 2, outer=i < 2))
    diffs = call(
        pool_kernel,
        [((groups, channels, rows), BF16)] * tp,
        own_at,
        pool_input,
        docs,
        news,
        *far_blocks,
    )
    diffs = list(diffs)
    for away in range(1, tp):
        turn = [(i, (i + away) % tp) for i in range(tp)]
        diffs[away] = (lax.ppermute(diffs[away], "tp", turn))
    (mapped,) = call(
        map_kernel,
        [((rows, groups * pool_map.shape[2]), BF16)],
        own_at,
        in_hbm(pool_map),
        in_hbm(pool_scale.reshape(1, -1)),
        *diffs,
    )
    far_mapped = to_twin(mapped)
    gains = (in_hbm(mix_gain.reshape(1, -1)), in_hbm(ffn_gain.reshape(1, -1)))
    table = functools.partial(table_kernel, capacity, skip)
    tables = [((slots, rows), BF16), ((rows, slots), BF16, True)]
    own_pick, own_weight = call(table, tables, own_at, news)
    far_pick, far_weight = call(table, tables, far_at, news)

    def there(x):
        columns = x.shape[1]
        x = x.reshape(experts, capacity, columns)
        return (lax.all_to_all(x, HALF, 0, 0, tiled=True).reshape(-1, columns))

    big = 24 * 2**20
    own_send, stream = call(
        send_kernel,
        [((slots, width), BF16, True), ((rows, width), BF16, True)],
        own_at, mapped, w_out, *gains, own_pick, residual,
        vmem=big,
    )
    own_in = there(own_send)
    (far_send,) = call(
        send_kernel,
        [((slots, width), BF16, True)],
        far_at, far_mapped, w_out, *gains, far_pick, *far_pieces,
        vmem=big,
    )
    far_in = there(far_send)
    part = width // 2
    *own_outs, _ = expert_rows(own_in, w_gate, w_up, w_down, 2, part)
    far_out_0, far_hidden = expert_rows(far_in, w_gate, w_up, w_down, 1, part)
    far_out_1 = down_rows(far_hidden, w_down, part)
    others, own_sums = [], []
    for outs in zip((far_out_0, far_out_1), own_outs):
        far_back = there(outs[0])
        (far_part,) = call(
            sum_kernel,
            [((rows, part), BF16)],
            far_weight, far_back,
            vmem=big,
        )
        others.append(to_twin(far_part))
        own_back = there(outs[1])
        own_sums += call(
            sum_kernel,
            [((rows, part), F32)],
            own_weight, own_back,
            vmem=big,
        )
    step = rows // 4
    inputs = [*own_sums, *others, stream, in_hbm(out_gain.reshape(1, -1))]
    specs = [pl.BlockSpec((step, v.shape[1]), lambda i: (i, 0)) for v in inputs[:-1]]
    out = pl.pallas_call(
        last_kernel,
        grid=(rows // step,),
        out_shape=jax.ShapeDtypeStruct((rows, width), BF16),
        in_specs=specs + [pl.BlockSpec((1, width), lambda i: (0, 0))],
        out_specs=pl.BlockSpec((step, width), lambda i: (i, 0)),
        compiler_params=pltpu.CompilerParams(vmem_limit_bytes=16 * 2**20),
    )(*inputs)
    return out


def solution(mesh):
    sp, tp = mesh.shape["sp"], mesh.shape["tp"]
    planes = 2 if sp % 4 == 0 else 1
    fine = Mesh(mesh.devices.reshape(2, planes, sp // (2 * planes), tp), ALL)
    rowwise = P(ALL, None)
    each = P(ALL, None, None)
    in_specs = (
        P(None, "tp", SP),
        P(SP),
        P(),
        P(),
        P(),
        rowwise,
        P(),
        P(),
        P(),
        rowwise,
        rowwise,
        each,
        each,
        each,
    )

    return jax.shard_map(local, mesh=fine, in_specs=in_specs, out_specs=rowwise, check_vma=False)
```
